32 devices in a mesh: fs: 4 (over z), tp: 8 (over y, x, core).
Axes of the slice: x: 2, y: 2, z: 4, core: 2. Of those that a mesh axis runs over, the one named last changes fastest.
Arguments:
- block_in: bfloat16 [4096, 2304], P('fs'), may hold values from -6 to 6
- out_cot: bfloat16 [4096, 2304], P('fs'), may hold values from -6 to 6
- gated_out: bfloat16 [4096, 4608], P('fs', 'tp'), may hold values from -6 to 6
- gate_cot: bfloat16 [4096, 4608], P('fs', 'tp'), may hold values from -6 to 6
- factor_out: bfloat16 [2304, 192], P('fs'), may hold values from -0.104166667 to 0.104166667
- factor_z: bfloat16 [2304, 192], P('fs'), may hold values from -0.104166667 to 0.104166667
- weight_out: float32 [4608, 2304], P('tp', 'fs'), may hold values from -0.09375 to 0.09375
- weight_z: float32 [2304, 4608], P('fs', 'tp'), may hold values from -0.125 to 0.125
- first_out: float32 [4608, 192], P('tp', 'fs'), may hold values from -512 to 512
- second_out: float32 [4608, 192], P('tp', 'fs'), may hold values from 819.2 to 20480
- first_z: float32 [192, 4608], P('fs', 'tp'), may hold values from -512 to 512
- second_z: float32 [192, 4608], P('fs', 'tp'), may hold values from 819.2 to 20480
Outputs:
- step_out: float32 [4608, 2304], P('tp', 'fs')
- step_z: float32 [2304, 4608], P('fs', 'tp')
- new_first_out: float32 [4608, 192], P('tp', 'fs')
- new_second_out: float32 [4608, 192], P('tp', 'fs')
- new_first_z: float32 [192, 4608], P('fs', 'tp')
- new_second_z: float32 [192, 4608], P('fs', 'tp')
- copy_out: bfloat16 [4608, 2304], P('tp')
- copy_z: bfloat16 [2304, 4608], P(None, 'tp')
The draws below stay inside these ranges and needn't reach their ends.
All inputs are finite; a program needn't handle non-finite values.
Results may differ from the reference program's by a relative error of at most 0.0018.
Values may be sent and summed in bfloat16 or wider, within the bound.
A program may use at most 64 MiB of HBM per device.

```python
import math
import jax
import jax.numpy as jnp
from jax import lax

D = 2304
INNER = 4608
RANK = 192
TOKENS = 4096


def shared_parts(key, member):
    folded = jax.random.fold_in(key, 1000 + member)
    subkeys = jax.random.split(folded, 4)
    width_dir = jnp.clip(jax.random.normal(subkeys[0], (D,), jnp.float32), -3.0, 3.0)
    inner_dir = jnp.clip(jax.random.normal(subkeys[1], (INNER,), jnp.float32), -3.0, 3.0)
    rank_wts = jax.random.uniform(subkeys[2], (RANK,), jnp.float32, 0.5, 1.5)
    token_sign = (2 * jax.random.randint(subkeys[3], (TOKENS,), 0, 2) - 1).astype(jnp.float32)
    return (width_dir, inner_dir, rank_wts, token_sign)


def noise_field(key, label_code, array_shape, clip_bound):
    subkey = jax.random.fold_in(key, label_code)
    return jnp.clip(jax.random.normal(subkey, array_shape, jnp.float32), -clip_bound, clip_bound)


def coupling_level():
    return min(math.sqrt(15.0 / math.sqrt(D * TOKENS)), 0.5)


def token_field(key, member, label_code, use_width):
    width_dir, inner_dir, rank_wts, token_sign = shared_parts(key, member)
    if use_width:
        common_dir = width_dir
        columns = D
    else:
        common_dir = inner_dir
        columns = INNER
    drawn = noise_field(key, label_code, (TOKENS, columns), 4.0)
    drawn = drawn + coupling_level() * token_sign[:, None] * common_dir[None, :]
    return jnp.clip(drawn, -6.0, 6.0).astype(jnp.bfloat16)


def factor_field(key, member, label_code):
    width_dir, inner_dir, rank_wts, token_sign = shared_parts(key, member)
    spread = D ** (-0.5)
    drawn = spread * noise_field(key, label_code, (D, RANK), 4.0)
    drawn = drawn + 0.1 * spread * width_dir[:, None] * rank_wts[None, :]
    return jnp.clip(drawn, -5.0 * spread, 5.0 * spread).astype(jnp.bfloat16)


def draw_block_in(key, part):
    return token_field(key, 2, 11, True)


def draw_gate_cot(key, part):
    return token_field(key, 2, 12, False)


def draw_out_cot(key, part):
    return token_field(key, 1, 13, True)


def draw_gated_out(key, part):
    return token_field(key, 1, 14, False)


def draw_factor_out(key, part):
    return factor_field(key, 1, 15)


def draw_factor_z(key, part):
    return factor_field(key, 2, 16)


def draw_first_out(key, part):
    width_dir, inner_dir, rank_wts, token_sign = shared_parts(key, 1)
    root_tokens = math.sqrt(TOKENS)
    drawn = noise_field(key, 17, (INNER, RANK), 4.0) + 0.8 * inner_dir[:, None] * rank_wts[None, :]
    return jnp.clip(root_tokens * drawn, -8.0 * root_tokens, 8.0 * root_tokens)


def draw_first_z(key, part):
    width_dir, inner_dir, rank_wts, token_sign = shared_parts(key, 2)
    root_tokens = math.sqrt(TOKENS)
    drawn = noise_field(key, 18, (RANK, INNER), 4.0) + 0.8 * rank_wts[:, None] * inner_dir[None, :]
    return jnp.clip(root_tokens * drawn, -8.0 * root_tokens, 8.0 * root_tokens)


def level_of(own_key, extent, pieces, low, high):
    loudness, own = 1.0, jax.random.fold_in(own_key, 6)
    for position, blocks in pieces:
        draws = jnp.exp(jax.random.uniform(jax.random.fold_in(own, position), (blocks,), jnp.float32, low / len(pieces), high / len(pieces)))
        loudness = loudness * jnp.repeat(draws, extent[position] // blocks).reshape([-1 if axis == position else 1 for axis in range(len(extent))])
    return loudness


def scatter_about(own_key, dims, scale, reach, cuts=(), kind=jnp.bfloat16):
    result = scale * jax.random.normal(own_key, dims, jnp.float32)
    if cuts:
        result = result * level_of(own_key, dims, cuts, -0.22, 0.18)
    return jnp.clip(result, -reach, reach).astype(kind)


def setup_inputs(seed: int = 0) -> dict:
    key_list = jax.random.split(jax.random.key(seed), 13)
    return {
        "block_in": draw_block_in(jax.random.fold_in(key_list[12], 71), 0),
        "out_cot": draw_out_cot(jax.random.fold_in(key_list[12], 71), 0),
        "gated_out": draw_gated_out(jax.random.fold_in(key_list[12], 71), 0),
        "gate_cot": draw_gate_cot(jax.random.fold_in(key_list[12], 71), 0),
        "factor_out": draw_factor_out(jax.random.fold_in(key_list[12], 71), 0),
        "factor_z": draw_factor_z(jax.random.fold_in(key_list[12], 71), 0),
        "weight_out": scatter_about(key_list[6], (INNER, D), INNER ** -0.5, 0.09375, ((0, 8), (1, 4)), jnp.float32),
        "weight_z": scatter_about(key_list[7], (D, INNER), D ** -0.5, 0.125, ((0, 4), (1, 8)), jnp.float32),
        "first_out": draw_first_out(jax.random.fold_in(key_list[12], 71), 0),
        "second_out": jnp.clip(jnp.exp(math.log(20480.0) - 3.218876 * jax.random.uniform(key_list[9], (INNER, RANK), jnp.float32) ** level_of(key_list[9], (INNER, RANK), ((0, 8), (1, 4)), -0.2, 0.2)), 819.2, 20480.0),
        "first_z": draw_first_z(jax.random.fold_in(key_list[12], 71), 0),
        "second_z": jnp.clip(jnp.exp(math.log(20480.0) - 3.218876 * jax.random.uniform(key_list[11], (RANK, INNER), jnp.float32) ** level_of(key_list[11], (RANK, INNER), ((0, 4), (1, 8)), -0.2, 0.2)), 819.2, 20480.0),
    }


beta_first = 0.8
beta_second = 0.9
adam_eps = 1e-08
norm_eps = 1e-06
rate = 0.005

def moments(first, second, gradient):
    new_first = beta_first * first + (1.0 - beta_first) * gradient
    new_second = beta_second * second + (1.0 - beta_second) * gradient * gradient
    return (new_first, new_second, new_first / (jnp.sqrt(new_second) + adam_eps))

def reference(block_in, out_cot, gated_out, gate_cot, factor_out, factor_z, weight_out, weight_z, first_out, second_out, first_z, second_z):
    proj_cot = jnp.dot(out_cot.astype(jnp.float32), factor_out.astype(jnp.float32), precision=lax.Precision.HIGHEST)
    proj_input = jnp.dot(block_in.astype(jnp.float32), factor_z.astype(jnp.float32), precision=lax.Precision.HIGHEST)
    grad_out = jnp.dot(gated_out.astype(jnp.float32).T, proj_cot, precision=lax.Precision.HIGHEST)
    grad_z = jnp.dot(proj_input.T, gate_cot.astype(jnp.float32), precision=lax.Precision.HIGHEST)
    new_first_out, new_second_out, dir_out = moments(first_out, second_out, grad_out)
    new_first_z, new_second_z, dir_z = moments(first_z, second_z, grad_z)
    update_out = jnp.dot(dir_out, factor_out.astype(jnp.float32).T, precision=lax.Precision.HIGHEST)
    update_z = jnp.dot(factor_z.astype(jnp.float32), dir_z, precision=lax.Precision.HIGHEST)
    step_out = update_out * lax.rsqrt(jnp.mean(update_out * update_out) + norm_eps)
    step_z = update_z * lax.rsqrt(jnp.mean(update_z * update_z) + norm_eps)
    copy_out = (weight_out - rate * step_out).astype(jnp.bfloat16)
    copy_z = (weight_z - rate * step_z).astype(jnp.bfloat16)
    return (step_out, step_z, new_first_out, new_second_out, new_first_z, new_second_z, copy_out, copy_z)
```

```python
import functools

import jax
import jax.numpy as jnp
from jax import lax
from jax.experimental import pallas as pl
from jax.experimental.pallas import tpu as pltpu
from jax.sharding import PartitionSpec as P

beta_first = 0.8
beta_second = 0.9
adam_eps = 1e-08
norm_eps = 1e-06
rate = 0.005

MESH = pl.DeviceIdType.MESH
VMEM = pl.BlockSpec(memory_space=pltpu.VMEM)
PARTS = 4


def remote(src, dst, send, recv, **where):
    return pltpu.make_async_remote_copy(
        src_ref=src, dst_ref=dst, send_sem=send, recv_sem=recv, device_id=where, device_id_type=MESH
    )


def gather_kernel(fs, factor, full, send_z, recv_z, send_x, recv_x, send_c, recv_c, send_d, recv_d):
    me, mine = lax.axis_index("fs"), lax.axis_index("tp")
    part = lax.rem(mine, PARTS)
    far = mine + 2 - 4 * lax.rem(mine // 2, 2)
    near = mine + 1 - 2 * lax.rem(mine, 2)
    far_part = lax.rem(far, PARTS)
    barrier = pltpu.get_barrier_semaphore()
    for d in range(1, fs):
        pl.semaphore_signal(barrier, inc=1, device_id={"fs": lax.rem(me + d, fs)}, device_id_type=MESH)
    for other in (far, near):
        pl.semaphore_signal(barrier, inc=1, device_id={"tp": other}, device_id_type=MESH)
    pl.semaphore_wait(barrier, fs + 1)

    first, second, third, fourth = [], [], [], []
    for d in range(1, fs):
        copy = remote(
            factor.at[part], full.at[me, part], send_z.at[d - 1], recv_z.at[d - 1], fs=lax.rem(me + d, fs)
        )
        copy.start()
        first.append(copy)
    full[me] = factor[...]
    for d in range(1, fs):
        src = lax.rem(me - d + fs, fs)
        first[d - 1].wait_recv()
        block = full.at[src, part]
        copy = remote(block, block, send_x.at[d - 1], recv_x.at[d - 1], tp=far)
        copy.start()
        second.append(copy)
        copy = remote(block, block, send_c.at[d - 1], recv_c.at[d - 1], tp=near)
        copy.start()
        third.append(copy)
    for d in range(1, fs):
        src = lax.rem(me - d + fs, fs)
        second[d - 1].wait_recv()
        block = full.at[src, far_part]
        copy = remote(block, block, send_d.at[d - 1], recv_d.at[d - 1], tp=near)
        copy.start()
        fourth.append(copy)
    for copy in third + fourth:
        copy.wait_recv()
    for copy in first + second + third + fourth:
        copy.wait_send()


def gather_factors(fs, factors):
    parts, rows, columns = factors.shape
    dma = pltpu.SemaphoreType.DMA((fs - 1,))
    return pl.pallas_call(
        functools.partial(gather_kernel, fs),
        out_shape=jax.ShapeDtypeStruct((fs, parts, rows, columns), factors.dtype),
        in_specs=[VMEM],
        out_specs=VMEM,
        scratch_shapes=[dma] * 8,
        compiler_params=pltpu.CompilerParams(collective_id=0, has_side_effects=True),
        cost_estimate=pl.CostEstimate(flops=0, bytes_accessed=30_000_000, transcendentals=0),
    )(factors)


def reduce_kernel(
    fs, tp, term_out, term_z, first, second, full_out, full_z,
    new_first, new_second, dirs, high, low, total,
    arrived, partial, received, send_r, recv_r, send_g, recv_g, send_t, recv_t,
):
    me, mine = lax.axis_index("fs"), lax.axis_index("tp")
    terms = (term_out, term_z)
    fulls = (full_out, full_z)
    rank = first.shape[1]
    barrier = pltpu.get_barrier_semaphore()
    for d in range(1, fs):
        pl.semaphore_signal(barrier, inc=1, device_id={"fs": lax.rem(me + d, fs)}, device_id_type=MESH)
    for d in range(1, tp):
        pl.semaphore_signal(barrier, inc=1, device_id={"tp": lax.rem(mine + d, tp)}, device_id_type=MESH)
    pl.semaphore_wait(barrier, fs + tp - 2)

    sums = []
    for m in range(2):
        for d in range(1, fs):
            peer = lax.rem(me + d, fs)
            copy = remote(
                terms[m].at[peer], arrived.at[m, d - 1], send_r.at[m, d - 1], recv_r.at[m, d - 1], fs=peer
            )
            copy.start()
            sums.append(copy)
    gathers = []
    for m in range(2):
        gradient = terms[m][me]
        for d in range(1, fs):
            sums[m * (fs - 1) + d - 1].wait_recv()
            gradient = gradient + arrived[m, d - 1]
        moment = beta_first * first[m] + (1.0 - beta_first) * gradient
        square = beta_second * second[m] + (1.0 - beta_second) * gradient * gradient
        new_first[m] = moment
        new_second[m] = square
        dirs[m, me] = moment / (jnp.sqrt(square) + adam_eps)
        for d in range(1, fs):
            block = dirs.at[m, me]
            copy = remote(
                block, block, send_g.at[m, d - 1], recv_g.at[m, d - 1], fs=lax.rem(me + d, fs)
            )
            copy.start()
            gathers.append(copy)
    squares = []
    for m in range(2):
        for d in range(1, fs):
            gathers[m * (fs - 1) + d - 1].wait_recv()
        whole = jnp.concatenate([dirs[m, s] for s in range(fs)], axis=0)
        high_part = whole.astype(jnp.bfloat16)
        low_part = (whole - high_part.astype(jnp.float32)).astype(jnp.bfloat16)
        high[m] = high_part
        low[m] = low_part

        def body(s, acc):
            rows = fulls[m][s]
            update = jnp.dot(rows, high[m], preferred_element_type=jnp.float32)
            update = update + jnp.dot(rows, low[m], preferred_element_type=jnp.float32)
            return acc + jnp.sum(update * update, axis=0, keepdims=True)

        acc = lax.fori_loop(0, fs, body, jnp.zeros((1, whole.shape[1]), jnp.float32))
        squares.append(jnp.sum(acc))
    row = lax.broadcasted_iota(jnp.int32, partial.shape, 0)
    partial[...] = jnp.where(row == 0, squares[0], squares[1])
    totals = []
    for d in range(1, tp):
        copy = remote(
            partial, received.at[d - 1], send_t.at[d - 1], recv_t.at[d - 1], tp=lax.rem(mine + d, tp)
        )
        copy.start()
        totals.append(copy)
    result = partial[...]
    for d in range(1, tp):
        totals[d - 1].wait_recv()
        result = result + received[d - 1]
    total[...] = result
    for copy in sums + gathers + totals:
        copy.wait_send()


def reduce_moments(fs, tp, term_out, term_z, first, second, full_out, full_z):
    _, rank, inner = first.shape
    dma = pltpu.SemaphoreType.DMA
    shape = jax.ShapeDtypeStruct
    f32, bf16 = jnp.float32, jnp.bfloat16
    return pl.pallas_call(
        functools.partial(reduce_kernel, fs, tp),
        out_shape=(
            shape(first.shape, f32),
            shape(first.shape, f32),
            shape((2, fs, rank, inner), f32),
            shape((2, fs * rank, inner), bf16),
            shape((2, fs * rank, inner), bf16),
            shape((8, 128), f32),
        ),
        in_specs=[VMEM] * 6,
        out_specs=[VMEM] * 6,
        scratch_shapes=[
            pltpu.VMEM((2, fs - 1, rank, inner), f32),
            pltpu.VMEM((8, 128), f32),
            pltpu.VMEM((tp - 1, 8, 128), f32),
            dma((2, fs - 1)),
            dma((2, fs - 1)),
            dma((2, fs - 1)),
            dma((2, fs - 1)),
            dma((tp - 1,)),
            dma((tp - 1,)),
        ],
        compiler_params=pltpu.CompilerParams(
            collective_id=1, has_side_effects=True, vmem_limit_bytes=48 * 1024 * 1024
        ),
        cost_estimate=pl.CostEstimate(flops=0, bytes_accessed=100_000_000, transcendentals=0),
    )(term_out, term_z, first, second, full_out, full_z)


def copies_kernel(fs, own_out, own_z, all_out, all_z, kept, send_a, recv_a, send_b, recv_b):
    me = lax.axis_index("fs")
    barrier = pltpu.get_barrier_semaphore()

    @pl.when(me > 0)
    def _():
        pl.semaphore_signal(barrier, inc=1, device_id={"fs": me - 1}, device_id_type=MESH)

    @pl.when(me < fs - 1)
    def _():
        pl.semaphore_signal(barrier, inc=1, device_id={"fs": me + 1}, device_id_type=MESH)

    pl.semaphore_wait(barrier, jnp.minimum(me, 1) + jnp.minimum(fs - 1 - me, 1))

    owns, alls = (own_out, own_z), (all_out, all_z)
    local = [pltpu.make_async_copy(owns[m], alls[m].at[me], kept.at[m]) for m in range(2)]
    for copy in local:
        copy.start()

    def up(m, src, block, step):
        return remote(block, alls[m].at[src], send_a.at[m, step], recv_a.at[m, step], fs=me + 1)

    def down(m, src, block, step):
        return remote(block, alls[m].at[src], send_b.at[m, step], recv_b.at[m, step], fs=me - 1)

    for step in range(fs - 1):
        for m in range(2):
            below, above = me - step, me + step
            held_below = jnp.maximum(below, 0)
            held_above = jnp.minimum(above, fs - 1)
            if step > 0:
                @pl.when(below >= 0)
                def _(m=m, held_below=held_below, step=step):
                    block = alls[m].at[held_below]
                    up(m, held_below, block, step - 1).wait_recv()

                @pl.when(above < fs)
                def _(m=m, held_above=held_above, step=step):
                    block = alls[m].at[held_above]
                    down(m, held_above, block, step - 1).wait_recv()

            @pl.when((below >= 0) & (me < fs - 1))
            def _(m=m, held_below=held_below, step=step):
                block = owns[m] if step == 0 else alls[m].at[held_below]
                up(m, held_below, block, step).start()

            @pl.when((above < fs) & (me > 0))
            def _(m=m, held_above=held_above, step=step):
                block = owns[m] if step == 0 else alls[m].at[held_above]
                down(m, held_above, block, step).start()

    last = fs - 2
    for m in range(2):
        @pl.when(me - last - 1 >= 0)
        def _(m=m):
            up(m, 0, alls[m].at[0], last).wait_recv()

        @pl.when(me + last + 1 < fs)
        def _(m=m):
            down(m, 0, alls[m].at[0], last).wait_recv()

    for step in range(fs - 1):
        for m in range(2):
            @pl.when((me - step >= 0) & (me < fs - 1))
            def _(m=m, step=step):
                up(m, 0, owns[m], step).wait_send()

            @pl.when((me + step < fs) & (me > 0))
            def _(m=m, step=step):
                down(m, 0, owns[m], step).wait_send()
    for copy in local:
        copy.wait()


def gather_copies(fs, own_out, own_z):
    dma = pltpu.SemaphoreType.DMA((2, fs - 1))
    return pl.pallas_call(
        functools.partial(copies_kernel, fs),
        out_shape=tuple(jax.ShapeDtypeStruct((fs,) + own.shape, own.dtype) for own in (own_out, own_z)),
        in_specs=[VMEM] * 2,
        out_specs=[VMEM] * 2,
        scratch_shapes=[pltpu.SemaphoreType.DMA((2,)), dma, dma, dma, dma],
        compiler_params=pltpu.CompilerParams(collective_id=2, has_side_effects=True),
        cost_estimate=pl.CostEstimate(flops=0, bytes_accessed=100_000_000, transcendentals=0),
    )(own_out, own_z)


def split_parts(values):
    high_part = values.astype(jnp.bfloat16)
    low_part = (values - high_part.astype(jnp.float32)).astype(jnp.bfloat16)
    return (high_part, low_part)


def per_device(
    fs, tp,
    block_in, out_cot, gated_out, gate_cot, factor_out, factor_z,
    weight_out, weight_z, first_out, second_out, first_z, second_z,
):
    width, rank = factor_out.shape[0], factor_out.shape[1]
    inner = gated_out.shape[1]
    entries = width * fs * inner * tp

    both = jnp.concatenate([factor_out, factor_z], axis=1).reshape(PARTS, width // PARTS, 2 * rank)
    full = gather_factors(fs, both).reshape(width * fs, 2 * rank)
    full_out, full_z = full[:, :rank], full[:, rank:]

    def term(values, factor, other):
        proj = jnp.dot(values, factor, preferred_element_type=jnp.float32)
        high_part, low_part = split_parts(proj)
        return jnp.dot(high_part.T, other, preferred_element_type=jnp.float32) + jnp.dot(
            low_part.T, other, preferred_element_type=jnp.float32
        )

    term_out = term(out_cot, full_out, gated_out).reshape(fs, rank // fs, inner)
    term_z = term(block_in, full_z, gate_cot).reshape(fs, rank // fs, inner)
    new_first, new_second, _, high, low, total = reduce_moments(
        fs, tp, term_out, term_z,
        jnp.stack([first_out.T, first_z]), jnp.stack([second_out.T, second_z]),
        full_out.reshape(fs, width, rank), full_z.reshape(fs, width, rank),
    )
    scale_out = lax.rsqrt(total[0, 0] / entries + norm_eps)
    scale_z = lax.rsqrt(total[1, 0] / entries + norm_eps)
    pair = jnp.concatenate([high, low], axis=1)

    def twice(factor):
        return jnp.concatenate([factor, factor], axis=1)

    def of_out(factor):
        return lax.dot_general(
            pair[0], twice(factor), (((0,), (1,)), ((), ())), preferred_element_type=jnp.float32
        )

    def of_z(factor):
        return jnp.dot(twice(factor), pair[1], preferred_element_type=jnp.float32)

    step_out = of_out(factor_out) * scale_out
    step_z = of_z(factor_z) * scale_z
    fresh_out = (weight_out - rate * step_out).astype(jnp.bfloat16)
    fresh_z = (weight_z - rate * step_z).astype(jnp.bfloat16)
    copies_out, copies_z = gather_copies(fs, fresh_out, fresh_z)
    copy_out = copies_out.transpose(1, 0, 2).reshape(inner, fs * width)
    copy_z = copies_z.reshape(fs * width, inner)
    return (
        step_out, step_z,
        new_first[0].T, new_second[0].T, new_first[1], new_second[1],
        copy_out, copy_z,
    )


def solution(mesh):
    return jax.shard_map(
        functools.partial(per_device, mesh.shape["fs"], mesh.shape["tp"]),
        mesh=mesh,
        in_specs=(
            P("fs", None),
            P("fs", None),
            P("fs", "tp"),
            P("fs", "tp"),
            P("fs", None),
            P("fs", None),
            P("tp", "fs"),
            P("fs", "tp"),
            P("tp", "fs"),
            P("tp", "fs"),
            P("fs", "tp"),
            P("fs", "tp"),
        ),
        out_specs=(
            P("tp", "fs"),
            P("fs", "tp"),
            P("tp", "fs"),
            P("tp", "fs"),
            P("fs", "tp"),
            P("fs", "tp"),
            P("tp", None),
            P(None, "tp"),
        ),
        check_vma=False,
    )
```

```python
import functools

import jax
import jax.numpy as jnp
from jax import lax
from jax.experimental import pallas as pl
from jax.experimental.pallas import tpu as pltpu
from jax.sharding import PartitionSpec as P

beta_first = 0.8
beta_second = 0.9
adam_eps = 1e-08
norm_eps = 1e-06
rate = 0.005


MESH = pl.DeviceIdType.MESH
VMEM = pl.BlockSpec(memory_space=pltpu.VMEM)
PARTS = 4


def remote(src, dst, send, recv, **where):
    return pltpu.make_async_remote_copy(
        src_ref=src, dst_ref=dst, send_sem=send, recv_sem=recv, device_id=where, device_id_type=MESH
    )


def gather_kernel(fs, factor, full, send_z, recv_z, send_x, recv_x, send_c, recv_c, send_d, recv_d):
    me, mine = lax.axis_index("fs"), lax.axis_index("tp")
    part = lax.rem(mine, PARTS)
    far = mine + 2 - 4 * lax.rem(mine // 2, 2)
    near = mine + 1 - 2 * lax.rem(mine, 2)
    far_part = lax.rem(far, PARTS)
    barrier = pltpu.get_barrier_semaphore()
    for d in range(1, fs):
        pl.semaphore_signal(barrier, inc=1, device_id={"fs": lax.rem(me + d, fs)}, device_id_type=MESH)
    for other in (far, near):
        pl.semaphore_signal(barrier, inc=1, device_id={"tp": other}, device_id_type=MESH)
    pl.semaphore_wait(barrier, fs + 1)

    first, second, third, fourth = [], [], [], []
    for d in range(1, fs):
        copy = remote(
            factor.at[part], full.at[me, part], send_z.at[d - 1], recv_z.at[d - 1], fs=lax.rem(me + d, fs)
        )
        copy.start()
        first.append(copy)
    full[me] = factor[...]
    for d in range(1, fs):
        src = lax.rem(me - d + fs, fs)
        first[d - 1].wait_recv()
        block = full.at[src, part]
        copy = remote(block, block, send_x.at[d - 1], recv_x.at[d - 1], tp=far)
        copy.start()
        second.append(copy)
        copy = remote(block, block, send_c.at[d - 1], recv_c.at[d - 1], tp=near)
        copy.start()
        third.append(copy)
    for d in range(1, fs):
        src = lax.rem(me - d + fs, fs)
        second[d - 1].wait_recv()
        block = full.at[src, far_part]
        copy = remote(block, block, send_d.at[d - 1], recv_d.at[d - 1], tp=near)
        copy.start()
        fourth.append(copy)
    for copy in third + fourth:
        copy.wait_recv()
    for copy in first + second + third + fourth:
        copy.wait_send()


def gather_factors(fs, factors):
    parts, rows, columns = factors.shape
    dma = pltpu.SemaphoreType.DMA((fs - 1,))
    return pl.pallas_call(
        functools.partial(gather_kernel, fs),
        out_shape=jax.ShapeDtypeStruct((fs, parts, rows, columns), factors.dtype),
        in_specs=[VMEM],
        out_specs=VMEM,
        scratch_shapes=[dma] * 8,
        compiler_params=pltpu.CompilerParams(collective_id=0, has_side_effects=True),
        cost_estimate=pl.CostEstimate(flops=0, bytes_accessed=3_000_000, transcendentals=0),
    )(factors)


def reduce_kernel(
    fs, tp, term_out, term_z, first, second, full_out, full_z,
    new_first, new_second, dirs, high, low, total,
    arrived, partial, received, send_r, recv_r, send_g, recv_g, send_t, recv_t,
):
    me, mine = lax.axis_index("fs"), lax.axis_index("tp")
    terms = (term_out, term_z)
    fulls = (full_out, full_z)
    rank = first.shape[1]
    barrier = pltpu.get_barrier_semaphore()
    for d in range(1, fs):
        pl.semaphore_signal(barrier, inc=1, device_id={"fs": lax.rem(me + d, fs)}, device_id_type=MESH)
    for d in range(1, tp):
        pl.semaphore_signal(barrier, inc=1, device_id={"tp": lax.rem(mine + d, tp)}, device_id_type=MESH)
    pl.semaphore_wait(barrier, fs + tp - 2)

    sums = []
    for m in range(2):
        for d in range(1, fs):
            peer = lax.rem(me + d, fs)
            copy = remote(
                terms[m].at[peer], arrived.at[m, d - 1], send_r.at[m, d - 1], recv_r.at[m, d - 1], fs=peer
            )
            copy.start()
            sums.append(copy)
    gathers = []
    for m in range(2):
        gradient = terms[m][me]
        for d in range(1, fs):
            sums[m * (fs - 1) + d - 1].wait_recv()
            gradient = gradient + arrived[m, d - 1]
        moment = beta_first * first[m] + (1.0 - beta_first) * gradient
        square = beta_second * second[m] + (1.0 - beta_second) * gradient * gradient
        new_first[m] = moment
        new_second[m] = square
        dirs[m, me] = moment / (jnp.sqrt(square) + adam_eps)
        for d in range(1, fs):
            block = dirs.at[m, me]
            copy = remote(
                block, block, send_g.at[m, d - 1], recv_g.at[m, d - 1], fs=lax.rem(me + d, fs)
            )
            copy.start()
            gathers.append(copy)
    squares = []
    for m in range(2):
        for d in range(1, fs):
            gathers[m * (fs - 1) + d - 1].wait_recv()
        whole = jnp.concatenate([dirs[m, s] for s in range(fs)], axis=0)
        high_part = whole.astype(jnp.bfloat16)
        low_part = (whole - high_part.astype(jnp.float32)).astype(jnp.bfloat16)
        high[m] = high_part
        low[m] = low_part

        def body(s, acc):
            rows = fulls[m][s]
            update = jnp.dot(rows, high[m], preferred_element_type=jnp.float32)
            update = update + jnp.dot(rows, low[m], preferred_element_type=jnp.float32)
            return acc + jnp.sum(update * update, axis=0, keepdims=True)

        acc = lax.fori_loop(0, fs, body, jnp.zeros((1, whole.shape[1]), jnp.float32))
        squares.append(jnp.sum(acc))
    row = lax.broadcasted_iota(jnp.int32, partial.shape, 0)
    partial[...] = jnp.where(row == 0, squares[0], squares[1])
    totals = []
    for d in range(1, tp):
        copy = remote(
            partial, received.at[d - 1], send_t.at[d - 1], recv_t.at[d - 1], tp=lax.rem(mine + d, tp)
        )
        copy.start()
        totals.append(copy)
    result = partial[...]
    for d in range(1, tp):
        totals[d - 1].wait_recv()
        result = result + received[d - 1]
    total[...] = result
    for copy in sums + gathers + totals:
        copy.wait_send()


def reduce_moments(fs, tp, term_out, term_z, first, second, full_out, full_z):
    _, rank, inner = first.shape
    dma = pltpu.SemaphoreType.DMA
    shape = jax.ShapeDtypeStruct
    f32, bf16 = jnp.float32, jnp.bfloat16
    return pl.pallas_call(
        functools.partial(reduce_kernel, fs, tp),
        out_shape=(
            shape(first.shape, f32),
            shape(first.shape, f32),
            shape((2, fs, rank, inner), f32),
            shape((2, fs * rank, inner), bf16),
            shape((2, fs * rank, inner), bf16),
            shape((8, 128), f32),
        ),
        in_specs=[VMEM] * 6,
        out_specs=[VMEM] * 6,
        scratch_shapes=[
            pltpu.VMEM((2, fs - 1, rank, inner), f32),
            pltpu.VMEM((8, 128), f32),
            pltpu.VMEM((tp - 1, 8, 128), f32),
            dma((2, fs - 1)),
            dma((2, fs - 1)),
            dma((2, fs - 1)),
            dma((2, fs - 1)),
            dma((tp - 1,)),
            dma((tp - 1,)),
        ],
        compiler_params=pltpu.CompilerParams(
            collective_id=1, has_side_effects=True, vmem_limit_bytes=48 * 1024 * 1024
        ),
        cost_estimate=pl.CostEstimate(flops=0, bytes_accessed=10_000_000, transcendentals=0),
    )(term_out, term_z, first, second, full_out, full_z)


def copies_kernel(fs, own_out, own_z, all_out, all_z, kept, send_a, recv_a, send_b, recv_b):
    me = lax.axis_index("fs")
    barrier = pltpu.get_barrier_semaphore()

    @pl.when(me > 0)
    def _():
        pl.semaphore_signal(barrier, inc=1, device_id={"fs": me - 1}, device_id_type=MESH)

    @pl.when(me < fs - 1)
    def _():
        pl.semaphore_signal(barrier, inc=1, device_id={"fs": me + 1}, device_id_type=MESH)

    pl.semaphore_wait(barrier, jnp.minimum(me, 1) + jnp.minimum(fs - 1 - me, 1))

    owns, alls = (own_out, own_z), (all_out, all_z)
    local = [pltpu.make_async_copy(owns[m], alls[m].at[me], kept.at[m]) for m in range(2)]
    for copy in local:
        copy.start()

    def up(m, src, block, step):
        return remote(block, alls[m].at[src], send_a.at[m, step], recv_a.at[m, step], fs=me + 1)

    def down(m, src, block, step):
        return remote(block, alls[m].at[src], send_b.at[m, step], recv_b.at[m, step], fs=me - 1)

    for step in range(fs - 1):
        for m in range(2):
            below, above = me - step, me + step
            held_below = jnp.maximum(below, 0)
            held_above = jnp.minimum(above, fs - 1)
            if step > 0:
                @pl.when(below >= 0)
                def _(m=m, held_below=held_below, step=step):
                    block = alls[m].at[held_below]
                    up(m, held_below, block, step - 1).wait_recv()

                @pl.when(above < fs)
                def _(m=m, held_above=held_above, step=step):
                    block = alls[m].at[held_above]
                    down(m, held_above, block, step - 1).wait_recv()

            @pl.when((below >= 0) & (me < fs - 1))
            def _(m=m, held_below=held_below, step=step):
                block = owns[m] if step == 0 else alls[m].at[held_below]
                up(m, held_below, block, step).start()

            @pl.when((above < fs) & (me > 0))
            def _(m=m, held_above=held_above, step=step):
                block = owns[m] if step == 0 else alls[m].at[held_above]
                down(m, held_above, block, step).start()

    last = fs - 2
    for m in range(2):
        @pl.when(me - last - 1 >= 0)
        def _(m=m):
            up(m, 0, alls[m].at[0], last).wait_recv()

        @pl.when(me + last + 1 < fs)
        def _(m=m):
            down(m, 0, alls[m].at[0], last).wait_recv()

    for step in range(fs - 1):
        for m in range(2):
            @pl.when((me - step >= 0) & (me < fs - 1))
            def _(m=m, step=step):
                up(m, 0, owns[m], step).wait_send()

            @pl.when((me + step < fs) & (me > 0))
            def _(m=m, step=step):
                down(m, 0, owns[m], step).wait_send()
    for copy in local:
        copy.wait()


def gather_copies(fs, own_out, own_z):
    dma = pltpu.SemaphoreType.DMA((2, fs - 1))
    return pl.pallas_call(
        functools.partial(copies_kernel, fs),
        out_shape=tuple(jax.ShapeDtypeStruct((fs,) + own.shape, own.dtype) for own in (own_out, own_z)),
        in_specs=[VMEM] * 2,
        out_specs=[VMEM] * 2,
        scratch_shapes=[pltpu.SemaphoreType.DMA((2,)), dma, dma, dma, dma],
        compiler_params=pltpu.CompilerParams(collective_id=2, has_side_effects=True),
        cost_estimate=pl.CostEstimate(flops=0, bytes_accessed=10_000_000, transcendentals=0),
    )(own_out, own_z)


def split_parts(values):
    high_part = values.astype(jnp.bfloat16)
    low_part = (values - high_part.astype(jnp.float32)).astype(jnp.bfloat16)
    return (high_part, low_part)


def per_device(
    fs, tp,
    block_in, out_cot, gated_out, gate_cot, factor_out, factor_z,
    weight_out, weight_z, first_out, second_out, first_z, second_z,
):
    width, rank = factor_out.shape[0], factor_out.shape[1]
    inner = gated_out.shape[1]
    entries = width * fs * inner * tp

    own_z = weight_z.astype(jnp.float16)
    others_z = [
        lax.ppermute(own_z, "fs", [(i, (i + d) % fs) for i in range(fs)]) for d in range(1, fs)
    ]

    both = jnp.concatenate([factor_out, factor_z], axis=1).reshape(PARTS, width // PARTS, 2 * rank)
    full = gather_factors(fs, both).reshape(width * fs, 2 * rank)
    full_out, full_z = full[:, :rank], full[:, rank:]

    def term(values, factor, other):
        proj = jnp.dot(values, factor, preferred_element_type=jnp.float32)
        high_part, low_part = split_parts(proj)
        return jnp.dot(high_part.T, other, preferred_element_type=jnp.float32) + jnp.dot(
            low_part.T, other, preferred_element_type=jnp.float32
        )

    term_out = term(out_cot, full_out, gated_out).reshape(fs, rank // fs, inner)
    term_z = term(block_in, full_z, gate_cot).reshape(fs, rank // fs, inner)
    new_first, new_second, _, high, low, total = reduce_moments(
        fs, tp, term_out, term_z,
        jnp.stack([first_out.T, first_z]), jnp.stack([second_out.T, second_z]),
        full_out.reshape(fs, width, rank), full_z.reshape(fs, width, rank),
    )
    scale_out = lax.rsqrt(total[0, 0] / entries + norm_eps)
    scale_z = lax.rsqrt(total[1, 0] / entries + norm_eps)
    pair = jnp.concatenate([high, low], axis=1)

    def twice(factor):
        return jnp.concatenate([factor, factor], axis=1)

    def of_out(factor):
        return lax.dot_general(
            pair[0], twice(factor), (((0,), (1,)), ((), ())), preferred_element_type=jnp.float32
        )

    def of_z(factor):
        return jnp.dot(twice(factor), pair[1], preferred_element_type=jnp.float32)

    step_out = of_out(factor_out) * scale_out
    step_z = of_z(factor_z) * scale_z
    fresh_out = (weight_out - rate * step_out).astype(jnp.bfloat16)
    halves = fresh_out.reshape(2, inner // 2, width)
    copies = gather_copies(fs, halves[0], halves[1])
    copy_out = jnp.concatenate([half.transpose(1, 0, 2).reshape(inner // 2, fs * width) for half in copies])
    me = lax.axis_index("fs")
    near_z = jnp.zeros((fs * width, inner), jnp.float16)
    for d, block in enumerate([own_z] + others_z):
        near_z = lax.dynamic_update_slice(near_z, block, (lax.rem(me - d + fs, fs) * width, 0))
    copy_z = (near_z.astype(jnp.float32) - (rate * scale_z) * of_z(full_z)).astype(jnp.bfloat16)
    return (
        step_out, step_z,
        new_first[0].T, new_second[0].T, new_first[1], new_second[1],
        copy_out, copy_z,
    )


def solution(mesh):
    return jax.shard_map(
        functools.partial(per_device, mesh.shape["fs"], mesh.shape["tp"]),
        mesh=mesh,
        in_specs=(
            P("fs", None),
            P("fs", None),
            P("fs", "tp"),
            P("fs", "tp"),
            P("fs", None),
            P("fs", None),
            P("tp", "fs"),
            P("fs", "tp"),
            P("tp", "fs"),
            P("tp", "fs"),
            P("fs", "tp"),
            P("fs", "tp"),
        ),
        out_specs=(
            P("tp", "fs"),
            P("fs", "tp"),
            P("tp", "fs"),
            P("tp", "fs"),
            P("fs", "tp"),
            P("fs", "tp"),
            P("tp", None),
            P(None, "tp"),
        ),
        check_vma=False,
    )
```
